768 devices in a mesh: sp: 16 (over y, core), dp: 48 (over z, x).
Axes of the slice: x: 4, y: 8, z: 12, core: 2. Of those that a mesh axis runs over, the one named last changes fastest.
Arguments:
- stream: bfloat16 [48, 2048, 2064], P('dp', 'sp'), may hold values from -6 to 6
- mix_gain: float32 [2064], replicated, may hold values from 0.1 to 1.9
- query_weight: bfloat16 [2064, 2048], P('dp'), may hold values from -0.125 to 0.125
- query_gain: float32 [128], replicated, may hold values from 0.1 to 1.9
- keys: bfloat16 [48, 2048, 512], P('dp', 'sp'), may hold values from -6 to 6
- key_gain: float32 [128], replicated, may hold values from 0.1 to 1.9
- values: bfloat16 [48, 2048, 512], P('dp', 'sp'), may hold values from -48 to 48
- stick_offset: float32 [16], replicated, may hold values from -8.5 to -7, as said below
Outputs:
- attended: bfloat16 [48, 2048, 2048], P('dp', 'sp')
The draws below stay inside these ranges and needn't reach their ends.
Inputs may be any that keep to these rules, and one draw needn't show every extreme that they name: `stick_offset`: one offset for each query head, added to all of that head's scores.
All inputs are finite; a program needn't handle non-finite values.
Results may differ from the reference program's by a relative error of at most 0.012.
Values may be sent and summed in bfloat16 or wider, within the bound.
No kernel may reach another device: no remote copies, remote signals or barrier semaphores. Data moves between devices by JAX's collectives and lax.ppermute only.
A program may use at most 64 MiB of HBM per device.

```python
import math
import jax
import jax.numpy as jnp
from jax import lax

D = 2064
QUERY_HEADS = 16
KV_HEADS = 4
HEAD_DIM = 128
LENGTH = 2048
SEQS = 48


def draw_stick_offset(key, part):
    base = jax.random.fold_in(key, 7)
    first_key, second_key = jax.random.split(base, 2)
    return jax.random.uniform(second_key, (QUERY_HEADS,), jnp.float32, -8.5, -7.0)


def level_of(rng, extent, shards, low, largest):
    level, own = 1.0, jax.random.fold_in(rng, 6)
    for position, shards_of in shards:
        heights = jnp.exp(jax.random.uniform(jax.random.fold_in(own, position), (shards_of,), jnp.float32, low / len(shards), largest / len(shards)))
        level = level * jnp.repeat(heights, extent[position] // shards_of).reshape([-1 if axis == position else 1 for axis in range(len(extent))])
    return level


def bell_draw(own_key, dims, deviation, most, pieces=(), kind=jnp.bfloat16):
    level = level_of(own_key, dims, pieces, -0.22, 0.18) if pieces else 1.0
    entries = jax.random.normal(own_key, dims, jnp.float32) * deviation * level
    return jnp.minimum(jnp.maximum(entries, -most), most).astype(kind)


def setup_inputs(seed: int = 0) -> dict:
    key_of = jax.random.split(jax.random.key(seed), 9)
    return {
        "stream": bell_draw(key_of[0], (SEQS, LENGTH, D), 1.0, 6.0, ((0, 48), (1, 16))),
        "mix_gain": jnp.clip(1.0 + 0.18 * jax.random.normal(key_of[1], (D,), jnp.float32), 0.1, 1.9),
        "query_weight": bell_draw(key_of[2], (D, QUERY_HEADS * HEAD_DIM), D ** -0.5, 0.125, ((0, 48),)),
        "query_gain": jnp.clip(1.0 + 0.18 * jax.random.normal(key_of[3], (HEAD_DIM,), jnp.float32), 0.1, 1.9),
        "keys": bell_draw(key_of[4], (SEQS, LENGTH, KV_HEADS * HEAD_DIM), 1.0, 6.0, ((0, 48), (1, 16))),
        "key_gain": jnp.clip(1.0 + 0.18 * jax.random.normal(key_of[5], (HEAD_DIM,), jnp.float32), 0.1, 1.9),
        "values": bell_draw(key_of[6], (SEQS, LENGTH, KV_HEADS * HEAD_DIM), 8.0, 48.0, ((0, 48), (1, 16))),
        "stick_offset": draw_stick_offset(jax.random.fold_in(key_of[8], 71), 0),
    }


norm_eps = 1e-06
row_block = 512

def rms_scaled(inputs, gain):
    wide = inputs.astype(jnp.float32)
    scaled = wide * lax.rsqrt(lax.optimization_barrier(jnp.mean(wide * wide, axis=-1, keepdims=True)) + norm_eps) * gain
    return scaled.astype(jnp.bfloat16)

def stick_weights(scores, first_row):
    rows_here = scores.shape[-2]
    keys_here = scores.shape[-1]
    query_pos = first_row + jnp.arange(rows_here, dtype=jnp.int32)
    key_pos = jnp.arange(keys_here, dtype=jnp.int32)
    causal = key_pos[None, :] < query_pos[:, None]
    log_keep = jnp.where(causal, jax.nn.log_sigmoid(-scores), 0.0)
    tail = lax.cumsum(log_keep, axis=scores.ndim - 1, reverse=True) - log_keep
    return jnp.where(causal, jnp.exp(jax.nn.log_sigmoid(scores) + tail), 0.0)

def head_output(query_rows, key_rows, value_rows, offset):
    seq_length = query_rows.shape[0]
    block = math.gcd(seq_length, row_block)
    outputs = []
    for block_id in range(seq_length // block):
        first = block_id * block
        finish = first + block
        scores = jnp.dot(query_rows[first:finish], key_rows[:finish].T, preferred_element_type=jnp.float32)
        scores = scores * HEAD_DIM ** (-0.5) + offset
        weights = stick_weights(scores, first).astype(jnp.bfloat16)
        outputs.append(jnp.dot(weights, value_rows[:finish], preferred_element_type=jnp.float32))
    return jnp.concatenate(outputs, axis=0).astype(jnp.bfloat16)

def reference(stream, mix_gain, query_weight, query_gain, keys, key_gain, values, stick_offset):
    group_size = QUERY_HEADS // KV_HEADS

    def one_sequence(inputs):
        stream_rows, key_rows, value_rows = inputs
        normed = rms_scaled(stream_rows, mix_gain)
        queries = jnp.dot(normed, query_weight, preferred_element_type=jnp.float32).astype(jnp.bfloat16)
        queries = lax.optimization_barrier(queries)
        query_heads = rms_scaled(queries.reshape(LENGTH, QUERY_HEADS, HEAD_DIM), query_gain)
        key_heads = rms_scaled(key_rows.reshape(LENGTH, KV_HEADS, HEAD_DIM), key_gain)
        value_heads = value_rows.reshape(LENGTH, KV_HEADS, HEAD_DIM)

        def one_head(head_id):
            kv_id = head_id // group_size
            query_one = lax.dynamic_index_in_dim(query_heads, head_id, 1, keepdims=False)
            key_one = lax.dynamic_index_in_dim(key_heads, kv_id, 1, keepdims=False)
            value_one = lax.dynamic_index_in_dim(value_heads, kv_id, 1, keepdims=False)
            return head_output(query_one, key_one, value_one, stick_offset[head_id])
        outputs = lax.map(one_head, jnp.arange(QUERY_HEADS, dtype=jnp.int32))
        return outputs.transpose(1, 0, 2).reshape(LENGTH, QUERY_HEADS * HEAD_DIM)
    return lax.map(one_sequence, (stream, keys, values))
```

```python
import jax
import jax.numpy as jnp
from jax import lax
from jax.experimental import pallas as pl
from jax.experimental.pallas import tpu as pltpu
from jax.sharding import Mesh, PartitionSpec as P


norm_eps = 1e-06
log2_e = 1.4426950408889634
tile = 256
low_y, cores, low_x = 2, 2, 4
group = low_y * cores


def block_step(k, v_t, q, upper, offset, carry, mask):
    scores = jnp.dot(k, q, preferred_element_type=jnp.float32) + offset
    keep = jnp.log2(1.0 + jnp.exp2(scores))
    if mask is not None:
        keep = jnp.where(mask, keep, 0.0)
    tail = jnp.dot(upper, keep.astype(jnp.bfloat16), preferred_element_type=jnp.float32)
    weights = jnp.exp2((scores - keep) - (tail + carry))
    if mask is not None:
        weights = jnp.where(mask, weights, 0.0)
    part = jnp.dot(v_t, weights.astype(jnp.bfloat16), preferred_element_type=jnp.float32)
    return part, carry + (tail[0:1] + keep[0:1])


def attend_kernel(
    place, offsets, w_own, w_left, w_right, w_low, w_high, x_own, x_core, x_far, x_both,
    kv_own, kv_one, kv_two, kv_three, gain, out, q_rows, total, carries,
):
    part, chip, core, column = place[0], place[1], place[2], place[3]
    member = chip * cores + core
    head_width = gain.shape[0]
    heads = offsets.shape[0]
    span = w_own.shape[0]
    half_span = w_low.shape[0]
    queries = None
    sources = ((w_own, 0, 0), (w_left, 3, 0), (w_right, 1, 0), (w_low, 2, 0), (w_high, 2, half_span))
    for weight, shift, begin in sources:
        start = pl.multiple_of(lax.rem(column + shift, low_x) * span + begin, 16)
        rows = pl.ds(start, weight.shape[0])
        own, near, far, both = x_own[rows], x_core[rows], x_far[rows], x_both[rows]
        flip = core == 0
        wide = jnp.concatenate(
            [
                jnp.where(flip, own, near),
                jnp.where(flip, near, own),
                jnp.where(flip, far, both),
                jnp.where(flip, both, far),
            ],
            axis=1,
        )
        term = lax.dot_general(
            weight[...], wide, (((0,), (0,)), ((), ())), preferred_element_type=jnp.float32
        )
        queries = term if queries is None else queries + term
    for h in range(heads):
        for t in range(2):
            rows = queries[h * head_width : (h + 1) * head_width, t * tile : (t + 1) * tile]
            rows = rows.astype(jnp.bfloat16).astype(jnp.float32)
            mean = jnp.mean(rows * rows, axis=0, keepdims=True)
            scaled = rows * lax.rsqrt(mean + norm_eps) * gain[:, 0:1]
            q_rows[jnp.bitwise_xor(chip, t), h] = scaled.astype(jnp.bfloat16)
    row_id = lax.broadcasted_iota(jnp.int32, (tile, tile), 0)
    column_id = lax.broadcasted_iota(jnp.int32, (tile, tile), 1)
    upper = (column_id > row_id).astype(jnp.float32).astype(jnp.bfloat16)
    mask = row_id < column_id

    def block_of(kv, index):
        left = kv[jnp.bitwise_xor(2 * index, member)]
        right = kv[jnp.bitwise_xor(2 * index + 1, member)]
        k = jnp.concatenate([left[0], right[0]], axis=0)
        return k, jnp.concatenate([left[1], right[1]], axis=1)

    zero = jnp.zeros((1, tile), jnp.float32)
    first, last = block_of(kv_own, 0), block_of(kv_own, 1)
    for h in range(heads):
        offset = offsets[h]
        piece, carry = block_step(*last, q_rows[1, h], upper, offset, zero, mask)
        more, carry = block_step(*first, q_rows[1, h], upper, offset, carry, None)
        total[h, 1] = piece + more
        carries[h, 1] = jnp.broadcast_to(carry, (8, tile))
        piece, carry = block_step(*first, q_rows[0, h], upper, offset, zero, mask)
        total[h, 0] = piece
        carries[h, 0] = jnp.broadcast_to(carry, (8, tile))

    for distance, kv in ((1, kv_one), (2, kv_two), (3, kv_three)):

        @pl.when(part >= distance)
        def _(kv=kv):
            blocks = (block_of(kv, 1), block_of(kv, 0))
            for h in range(heads):
                for t in range(2):
                    carry, summed = carries[h, t, 0:1], total[h, t]
                    for k, v_t in blocks:
                        piece, carry = block_step(
                            k, v_t, q_rows[t, h], upper, offsets[h], carry, None
                        )
                        summed = summed + piece
                    total[h, t] = summed
                    carries[h, t] = jnp.broadcast_to(carry, (8, tile))

    half = tile // 2
    for h in range(heads):
        for t in range(2):
            rows = total[h, t].T.astype(jnp.bfloat16)
            for c in range(2):
                out[2 * t + c, :, h * head_width : (h + 1) * head_width] = rows[
                    c * half : (c + 1) * half
                ]


def attend(place, offsets, weights, xs, kvs, gain):
    heads = offsets.shape[0]
    head_width = gain.shape[0]
    vmem = pl.BlockSpec(memory_space=pltpu.VMEM)
    smem = pl.BlockSpec(memory_space=pltpu.SMEM)
    flops = 2 * xs[0].size * heads * head_width * group
    flops += heads * 8 * 2 * tile * tile * (2 * head_width + tile)
    return pl.pallas_call(
        attend_kernel,
        out_shape=jax.ShapeDtypeStruct((group, tile // 2, heads * head_width), jnp.bfloat16),
        in_specs=[smem, smem, *[vmem] * 14],
        out_specs=vmem,
        scratch_shapes=[
            pltpu.VMEM((2, heads, head_width, tile), jnp.bfloat16),
            pltpu.VMEM((heads, 2, head_width, tile), jnp.float32),
            pltpu.VMEM((heads, 2, 8, tile), jnp.float32),
        ],
        cost_estimate=pl.CostEstimate(flops=flops, bytes_accessed=1 << 22, transcendentals=0),
    )(place, offsets, *weights, *xs, *kvs, gain)


def sent_to_all(value, axes):
    count = lax.axis_size(axes)
    copies = jnp.broadcast_to(value, (count, *value.shape))
    return lax.all_to_all(copies, axes, split_axis=0, concat_axis=0, tiled=True)


def swapped(value, axis):
    return lax.ppermute(value, axis, [(0, 1), (1, 0)])


def turned(value, axis, shift):
    count = lax.axis_size(axis)
    return lax.ppermute(value, axis, [(i, (i + shift) % count) for i in range(count)])


def flipped(value, bits):
    return lax.ppermute(value, ("yl", "core"), [(i, i ^ bits) for i in range(group)])


def handed_on(value, shift):
    count = lax.axis_size("yh")
    return lax.ppermute(value, "yh", [(i, i + shift) for i in range(count - shift)])


def layer(stream, mix_gain, query_weight, query_gain, keys, key_gain, values, stick_offset):
    part, chip, core = lax.axis_index("yh"), lax.axis_index("yl"), lax.axis_index("core")
    member = chip * cores + core
    head_width = query_gain.shape[0]
    heads_all = stick_offset.shape[0]
    heads = heads_all // group
    rows_dev = query_weight.shape[0]
    padded = -(-rows_dev // 16) * 16
    span = heads * head_width
    tokens = stream.shape[1]

    columns = lax.dynamic_slice_in_dim(query_weight, member * span, span, 1)
    columns = jnp.pad(columns, ((0, padded - rows_dev), (0, 0)))
    along_z = sent_to_all(columns, "z").reshape(-1, span)

    kv_heads = keys.shape[2] // head_width
    k = keys[0].reshape(tokens, kv_heads, head_width).astype(jnp.float32)
    k = k * lax.rsqrt(jnp.mean(k * k, axis=-1, keepdims=True) + norm_eps) * key_gain
    k = k.astype(jnp.bfloat16).transpose(1, 0, 2)
    v = values[0].reshape(tokens, kv_heads, head_width).transpose(1, 2, 0)
    kv = jnp.stack((k, v), axis=1)
    pieces = [lax.dynamic_index_in_dim(kv, member ^ bits, 0, keepdims=True) for bits in range(group)]
    pieces[1:] = [flipped(pieces[bits], bits) for bits in range(1, group)]
    kv_own = jnp.concatenate(pieces, axis=0)
    kvs = (kv_own, *[handed_on(kv_own, shift) for shift in range(1, lax.axis_size("yh"))])

    x_t = stream[0].T.astype(jnp.float32)
    scale = lax.rsqrt(jnp.mean(x_t * x_t, axis=0, keepdims=True) + norm_eps)
    normed = (x_t * scale * mix_gain[:, None]).astype(jnp.bfloat16)
    normed = normed.reshape(-1, low_x, rows_dev, tokens).transpose(1, 0, 2, 3)
    normed = jnp.pad(normed, ((0, 0), (0, 0), (0, padded - rows_dev), (0, 0)))
    normed = normed.reshape(-1, tokens)
    far = swapped(normed, "yl")
    near = swapped(normed, "core")
    xs = (normed, near, far, swapped(far, "core"))

    left, right = turned(along_z, "x", 1), turned(along_z, "x", -1)
    half = along_z.shape[0] // 2
    low, high = turned(left[:half], "x", 1), turned(right[half:], "x", -1)
    weights = (along_z, left, right, low, high)

    gain = query_gain * (head_width ** (-0.5) * log2_e)
    gain = jnp.broadcast_to(gain[:, None], (head_width, head_width))
    place = jnp.stack((part, chip, core, lax.axis_index("x"))).astype(jnp.int32)
    offsets = lax.dynamic_slice_in_dim(stick_offset * log2_e, member * heads, heads)
    attended = attend(place, offsets, weights, xs, kvs, gain)
    out = lax.all_to_all(attended, ("yl", "core"), split_axis=0, concat_axis=0, tiled=True)
    return out.transpose(1, 0, 2).reshape(1, tokens, heads_all * head_width)


def solution(mesh):
    sp, dp = mesh.shape["sp"], mesh.shape["dp"]
    fine = Mesh(
        mesh.devices.reshape(sp // group, low_y, cores, dp // low_x, low_x),
        ("yh", "yl", "core", "z", "x"),
    )
    along, across = ("yh", "yl", "core"), ("z", "x")
    return jax.shard_map(
        layer,
        mesh=fine,
        in_specs=(
            P(across, along, None),
            P(),
            P(across, None),
            P(),
            P(across, along, None),
            P(),
            P(across, along, None),
            P(),
        ),
        out_specs=P(across, along, None),
        check_vma=False,
    )
```

```python
import jax
import jax.numpy as jnp
from jax import lax
from jax.experimental import pallas as pl
from jax.experimental.pallas import tpu as pltpu
from jax.sharding import Mesh, PartitionSpec as P


norm_eps = 1e-06
log2_e = 1.4426950408889634
tile = 256
sublanes = 8
low_y, cores, low_x = 2, 2, 4
group = low_y * cores


def sub_step(k, q, offset, carry, mask):
    scores = jnp.dot(k, q, preferred_element_type=jnp.float32)
    lanes = scores.shape[1]
    sub = lax.broadcasted_iota(jnp.int32, (sublanes, lanes), 0)
    kept, pieces = None, []
    for i in range(scores.shape[0] // sublanes):
        rows = slice(i * sublanes, (i + 1) * sublanes)
        odds = jnp.exp2(scores[rows] + offset)
        if mask is not None:
            odds = jnp.where(mask[rows], odds, 0.0)
        keep = 1.0 / (1.0 + odds)
        piece = odds * keep
        pieces.append(piece if kept is None else piece * kept)
        kept = keep if kept is None else kept * keep
    for j in (1, 2, 4):
        kept = kept * jnp.where(sub < sublanes - j, pltpu.roll(kept, sublanes - j, 0), 1.0)
    later = jnp.where(sub < sublanes - 1, pltpu.roll(kept, sublanes - 1, 0), 1.0) * carry
    carry = carry * jnp.broadcast_to(kept[0:1], kept.shape)
    weights = jnp.concatenate([piece * later for piece in pieces], axis=0)
    return weights.astype(jnp.bfloat16), carry


def block_step(k, v_t, q, offset, carry, mask):
    half = tile // 2
    upper, carry = sub_step(k[half:], q, offset, carry, None if mask is None else mask[half:])
    lower, carry = sub_step(k[:half], q, offset, carry, None if mask is None else mask[:half])
    part = jnp.dot(v_t[:, half:], upper, preferred_element_type=jnp.float32)
    part += jnp.dot(v_t[:, :half], lower, preferred_element_type=jnp.float32)
    return part, carry


def attend_kernel(
    place, offsets, w_own, w_left, w_left_end, w_right, w_right_end, w_far, w_far_end, x_own, x_core, x_far, x_both,
    kv_own, kv_one, kv_two, kv_three, gain, out, q_rows, total, carries,
):
    part, chip, core, column = place[0], place[1], place[2], place[3]
    member = chip * cores + core
    head_width = gain.shape[0]
    heads = offsets.shape[0]
    span = w_own.shape[0]
    half_span = w_far.shape[0]
    queries = None
    sources = (
        (w_own, 0, 0),
        (w_left, 3, 0),
        (w_left_end, 3, half_span),
        (w_right, 1, 0),
        (w_right_end, 1, half_span),
        (w_far, 2, 0),
        (w_far_end, 2, half_span),
    )
    for weight, shift, begin in sources:
        start = pl.multiple_of(lax.rem(column + shift, low_x) * span + begin, 16)
        rows = pl.ds(start, weight.shape[0])
        own, near, far, both = x_own[rows], x_core[rows], x_far[rows], x_both[rows]
        flip = core == 0
        wide = jnp.concatenate(
            [
                jnp.where(flip, own, near),
                jnp.where(flip, near, own),
                jnp.where(flip, far, both),
                jnp.where(flip, both, far),
            ],
            axis=1,
        )
        term = lax.dot_general(
            weight[...], wide, (((0,), (0,)), ((), ())), preferred_element_type=jnp.float32
        )
        queries = term if queries is None else queries + term
    for h in range(heads):
        for t in range(2):
            rows = queries[h * head_width : (h + 1) * head_width, t * tile : (t + 1) * tile]
            rows = rows.astype(jnp.bfloat16).astype(jnp.float32)
            mean = jnp.mean(rows * rows, axis=0, keepdims=True)
            scaled = rows * lax.rsqrt(mean + norm_eps) * gain[:, 0:1]
            q_rows[jnp.bitwise_xor(chip, t), h] = scaled.astype(jnp.bfloat16)
    row_id = lax.broadcasted_iota(jnp.int32, (tile, tile), 0)
    column_id = lax.broadcasted_iota(jnp.int32, (tile, tile), 1)
    half = tile // 2
    inner = row_id % half
    depth = half // sublanes
    key_id = row_id - inner + (inner % sublanes) * depth + (depth - 1 - inner // sublanes)
    mask = key_id < column_id

    def block_of(kv, index):
        left = kv[jnp.bitwise_xor(2 * index, member)]
        right = kv[jnp.bitwise_xor(2 * index + 1, member)]
        k = jnp.concatenate([left[0], right[0]], axis=0)
        return k, jnp.concatenate([left[1], right[1]], axis=1)

    one = jnp.ones((sublanes, tile), jnp.float32)
    first, last = block_of(kv_own, 0), block_of(kv_own, 1)
    for h in range(heads):
        offset = offsets[h]
        piece, carry = block_step(*last, q_rows[1, h], offset, one, mask)
        more, carry = block_step(*first, q_rows[1, h], offset, carry, None)
        total[h, 1] = piece + more
        carries[h, 1] = carry
        piece, carry = block_step(*first, q_rows[0, h], offset, one, mask)
        total[h, 0] = piece
        carries[h, 0] = carry

    for distance, kv in ((1, kv_one), (2, kv_two), (3, kv_three)):

        @pl.when(part >= distance)
        def _(kv=kv):
            blocks = (block_of(kv, 1), block_of(kv, 0))
            for h in range(heads):
                for t in range(2):
                    carry, summed = carries[h, t], total[h, t]
                    for k, v_t in blocks:
                        piece, carry = block_step(
                            k, v_t, q_rows[t, h], offsets[h], carry, None
                        )
                        summed = summed + piece
                    total[h, t] = summed
                    carries[h, t] = carry

    for h in range(heads):
        for t in range(2):
            rows = total[h, t].T.astype(jnp.bfloat16)
            for c in range(2):
                out[2 * t + c, :, h * head_width : (h + 1) * head_width] = rows[
                    c * half : (c + 1) * half
                ]


def attend(place, offsets, weights, xs, kvs, gain):
    heads = offsets.shape[0]
    head_width = gain.shape[0]
    vmem = pl.BlockSpec(memory_space=pltpu.VMEM)
    smem = pl.BlockSpec(memory_space=pltpu.SMEM)
    flops = 2 * xs[0].size * heads * head_width * group
    flops += heads * 8 * 2 * tile * tile * (2 * head_width + tile)
    return pl.pallas_call(
        attend_kernel,
        out_shape=jax.ShapeDtypeStruct((group, tile // 2, heads * head_width), jnp.bfloat16),
        in_specs=[smem, smem, *[vmem] * 16],
        out_specs=vmem,
        scratch_shapes=[
            pltpu.VMEM((2, heads, head_width, tile), jnp.bfloat16),
            pltpu.VMEM((heads, 2, head_width, tile), jnp.float32),
            pltpu.VMEM((heads, 2, sublanes, tile), jnp.float32),
        ],
        cost_estimate=pl.CostEstimate(flops=flops, bytes_accessed=1 << 22, transcendentals=0),
    )(place, offsets, *weights, *xs, *kvs, gain)


def sent_to_all(value, axes):
    count = lax.axis_size(axes)
    copies = jnp.broadcast_to(value, (count, *value.shape))
    return lax.all_to_all(copies, axes, split_axis=0, concat_axis=0, tiled=True)


def swapped(value, axis):
    return lax.ppermute(value, axis, [(0, 1), (1, 0)])


def turned(value, axis, shift):
    count = lax.axis_size(axis)
    return lax.ppermute(value, axis, [(i, (i + shift) % count) for i in range(count)])


def flipped(value, bits):
    return lax.ppermute(value, ("yl", "core"), [(i, i ^ bits) for i in range(group)])


def handed_on(value, shift):
    count = lax.axis_size("yh")
    return lax.ppermute(value, "yh", [(i, i + shift) for i in range(count - shift)])


def layer(stream, mix_gain, query_weight, query_gain, keys, key_gain, values, stick_offset):
    part, chip, core = lax.axis_index("yh"), lax.axis_index("yl"), lax.axis_index("core")
    member = chip * cores + core
    head_width = query_gain.shape[0]
    heads_all = stick_offset.shape[0]
    heads = heads_all // group
    rows_dev = query_weight.shape[0]
    padded = -(-rows_dev // 16) * 16
    span = heads * head_width
    tokens = stream.shape[1]

    columns = lax.dynamic_slice_in_dim(query_weight, member * span, span, 1)
    columns = jnp.pad(columns, ((0, padded - rows_dev), (0, 0)))
    along_z = sent_to_all(columns, "z").reshape(-1, span)

    kv_heads = keys.shape[2] // head_width

    def spread(rows):
        return rows.reshape(sublanes, tokens // sublanes, -1)[:, ::-1].swapaxes(0, 1)

    k = spread(keys[0]).reshape(tokens, kv_heads, head_width).astype(jnp.float32)
    k = k * lax.rsqrt(jnp.mean(k * k, axis=-1, keepdims=True) + norm_eps) * key_gain
    k = k.astype(jnp.bfloat16).transpose(1, 0, 2)
    v = spread(values[0]).reshape(tokens, kv_heads, head_width).transpose(1, 2, 0)
    kv = jnp.stack((k, v), axis=1)
    pieces = [lax.dynamic_index_in_dim(kv, member ^ bits, 0, keepdims=True) for bits in range(group)]
    pieces[1:] = [flipped(pieces[bits], bits) for bits in range(1, group)]
    kv_own = jnp.concatenate(pieces, axis=0)
    kvs = (kv_own, *[handed_on(kv_own, shift) for shift in range(1, lax.axis_size("yh"))])

    x_t = stream[0].T.astype(jnp.float32)
    scale = lax.rsqrt(jnp.mean(x_t * x_t, axis=0, keepdims=True) + norm_eps)
    normed = (x_t * scale * mix_gain[:, None]).astype(jnp.bfloat16)
    normed = normed.reshape(-1, low_x, rows_dev, tokens).transpose(1, 0, 2, 3)
    normed = jnp.pad(normed, ((0, 0), (0, 0), (0, padded - rows_dev), (0, 0)))
    normed = normed.reshape(-1, tokens)
    far = swapped(normed, "yl")
    near = swapped(normed, "core")
    xs = (normed, near, far, swapped(far, "core"))

    half = along_z.shape[0] // 2
    top, bottom = along_z[:half], along_z[half:]
    left_top = turned(top, "x", 1)
    right_bottom = turned(bottom, "x", -1)
    left_bottom = turned(bottom, "x", 1)
    right_top = turned(top, "x", -1)
    far_top = turned(left_top, "x", 1)
    far_bottom = turned(right_bottom, "x", -1)
    weights = (along_z, left_top, left_bottom, right_top, right_bottom, far_top, far_bottom)

    gain = query_gain * (head_width ** (-0.5) * log2_e)
    gain = jnp.broadcast_to(gain[:, None], (head_width, head_width))
    place = jnp.stack((part, chip, core, lax.axis_index("x"))).astype(jnp.int32)
    offsets = lax.dynamic_slice_in_dim(stick_offset * log2_e, member * heads, heads)
    attended = attend(place, offsets, weights, xs, kvs, gain)
    out = lax.all_to_all(attended, ("yl", "core"), split_axis=0, concat_axis=0, tiled=True)
    return out.transpose(1, 0, 2).reshape(1, tokens, heads_all * head_width)


def solution(mesh):
    sp, dp = mesh.shape["sp"], mesh.shape["dp"]
    fine = Mesh(
        mesh.devices.reshape(sp // group, low_y, cores, dp // low_x, low_x),
        ("yh", "yl", "core", "z", "x"),
    )
    along, across = ("yh", "yl", "core"), ("z", "x")
    return jax.shard_map(
        layer,
        mesh=fine,
        in_specs=(
            P(across, along, None),
            P(),
            P(across, None),
            P(),
            P(across, along, None),
            P(),
            P(across, along, None),
            P(),
        ),
        out_specs=P(across, along, None),
        check_vma=False,
    )
```

```python
import jax
import jax.numpy as jnp
from jax import lax
from jax.experimental import pallas as pl
from jax.experimental.pallas import tpu as pltpu
from jax.sharding import Mesh, PartitionSpec as P


norm_eps = 1e-06
log2_e = 1.4426950408889634
tile = 256
sublanes = 8
low_y, cores, low_x = 2, 2, 4
group = low_y * cores


def sub_step(k, q, offset, carry, mask):
    scores = jnp.dot(k, q, preferred_element_type=jnp.float32)
    lanes = scores.shape[1]
    sub = lax.broadcasted_iota(jnp.int32, (sublanes, lanes), 0)
    kept, pieces = None, []
    for i in range(scores.shape[0] // sublanes):
        rows = slice(i * sublanes, (i + 1) * sublanes)
        odds = jnp.exp2(scores[rows] + offset)
        if mask is not None:
            odds = jnp.where(mask[rows], odds, 0.0)
        keep = 1.0 / (1.0 + odds)
        piece = odds * keep
        pieces.append(piece if kept is None else piece * kept)
        kept = keep if kept is None else kept * keep
    for j in (1, 2, 4):
        kept = kept * jnp.where(sub < sublanes - j, pltpu.roll(kept, sublanes - j, 0), 1.0)
    later = jnp.where(sub < sublanes - 1, pltpu.roll(kept, sublanes - 1, 0), 1.0) * carry
    carry = carry * jnp.broadcast_to(kept[0:1], kept.shape)
    weights = jnp.concatenate([piece * later for piece in pieces], axis=0)
    return weights.astype(jnp.bfloat16), carry


def block_step(k, v_t, q, offset, carry, mask):
    half = tile // 2
    upper, carry = sub_step(k[half:], q, offset, carry, None if mask is None else mask[half:])
    lower, carry = sub_step(k[:half], q, offset, carry, None if mask is None else mask[:half])
    part = jnp.dot(v_t[:, half:], upper, preferred_element_type=jnp.float32)
    part += jnp.dot(v_t[:, :half], lower, preferred_element_type=jnp.float32)
    return part, carry


def attend_rows(late, place, offsets, q_rows, kvs, arrivals, out, total, carries):
    part, core, member = place[0], place[1], place[3]
    heads, head_width = q_rows.shape[:2]
    half = tile // 2
    row_id = lax.broadcasted_iota(jnp.int32, (tile, tile), 0)
    column_id = lax.broadcasted_iota(jnp.int32, (tile, tile), 1)
    inner = row_id % half
    depth = half // sublanes
    key_id = row_id - inner + (inner % sublanes) * depth + (depth - 1 - inner // sublanes)

    def block_of(distance, index):
        left = kvs[distance, jnp.bitwise_xor(2 * index, member)]
        right = kvs[distance, jnp.bitwise_xor(2 * index + 1, member)]
        k = jnp.concatenate([left[0], right[0]], axis=0)
        return k, jnp.concatenate([left[1], right[1]], axis=1)

    def walk(blocks, mask):
        for h in range(heads):
            carry, summed = carries[h], total[h]
            for k, v_t in blocks:
                piece, carry = block_step(k, v_t, q_rows[h], offsets[h], carry, mask)
                summed = summed + piece
            total[h] = summed
            carries[h] = carry

    for h in range(heads):
        total[h] = jnp.zeros((head_width, tile), jnp.float32)
        carries[h] = jnp.ones((sublanes, tile), jnp.float32)
    arrivals[0].wait()

    @pl.when(late == 1)
    def _():
        walk([block_of(0, 1)], key_id < column_id)

    walk([block_of(0, 0)], key_id < column_id + late * tile)
    for distance in range(1, kvs.shape[0]):
        arrivals[distance].wait()

        @pl.when(part >= distance)
        def _(distance=distance):
            walk([block_of(distance, 1), block_of(distance, 0)], None)

    for h in range(heads):
        turned_back = total[h].T.astype(jnp.bfloat16)
        for c in range(cores):
            out[jnp.bitwise_xor(core, c), :, h * head_width : (h + 1) * head_width] = turned_back[
                c * half : (c + 1) * half
            ]


def first_kernel(
    place, offsets, w_own, w_left, w_left_end, w_right, w_right_end, w_far, w_far_end,
    x_far, x_both, x_own, x_near, kv_own, kv_one, kv_two, kv_three, gain,
    out, q_mine, q_rows, weight, rows, kvs, total, carries, done,
):
    core, column = place[1], place[2]
    heads, head_width = q_rows.shape[:2]
    span = w_own.shape[0]
    half_span = w_far.shape[0]
    half = tile // 2
    sources = (
        (w_own, 0, 0),
        (w_left, 3, 0),
        (w_left_end, 3, half_span),
        (w_right, 1, 0),
        (w_right_end, 1, half_span),
        (w_far, 2, 0),
        (w_far_end, 2, half_span),
    )
    moves = []
    for n, piece in enumerate((x_far, x_both, x_own, x_near)):
        place_at = (n // 2) * tile + jnp.bitwise_xor(core, n % 2) * half
        moves.append((piece, rows.at[:, pl.ds(pl.multiple_of(place_at, half), half)]))
    for piece, shift, begin in sources:
        start = pl.multiple_of(lax.rem(column + shift, low_x) * span + begin, 16)
        moves.append((piece, weight.at[pl.ds(start, piece.shape[0])]))
    first_kv = len(moves)
    for n, piece in enumerate((kv_own, kv_one, kv_two, kv_three)):
        moves.append((piece, kvs.at[n]))
    moves = [pltpu.make_async_copy(a, b, done.at[n]) for n, (a, b) in enumerate(moves)]
    for move in moves:
        move.start()
    for move in moves[:first_kv]:
        move.wait()
    queries = lax.dot_general(
        weight[...], rows[...], (((0,), (0,)), ((), ())), preferred_element_type=jnp.float32
    )
    for h in range(heads):
        for side, target in enumerate((q_rows, q_mine)):
            wide = queries[h * head_width : (h + 1) * head_width, side * tile : (side + 1) * tile]
            wide = wide.astype(jnp.bfloat16).astype(jnp.float32)
            mean = jnp.mean(wide * wide, axis=0, keepdims=True)
            scaled = wide * lax.rsqrt(mean + norm_eps) * gain[:, 0:1]
            target[h] = scaled.astype(jnp.bfloat16)
    late = 1 - place[4]
    attend_rows(late, place, offsets, q_rows, kvs, moves[first_kv:], out, total, carries)


def second_kernel(
    place, offsets, q_rows, kv_own, kv_one, kv_two, kv_three, out, kvs, total, carries, done
):
    moves = [
        pltpu.make_async_copy(piece, kvs.at[n], done.at[n])
        for n, piece in enumerate((kv_own, kv_one, kv_two, kv_three))
    ]
    for move in moves:
        move.start()
    attend_rows(place[4], place, offsets, q_rows, kvs, moves, out, total, carries)


vmem = pl.BlockSpec(memory_space=pltpu.VMEM)
smem = pl.BlockSpec(memory_space=pltpu.SMEM)
anywhere = pl.BlockSpec(memory_space=pl.ANY)


def estimate(heads, head_width, features):
    flops = 2 * features * 2 * tile * heads * head_width
    flops += heads * 8 * tile * tile * 4 * head_width
    return pl.CostEstimate(flops=flops, bytes_accessed=1 << 22, transcendentals=0)


def attend_first(place, offsets, weights, xs, kvs, gain):
    heads = offsets.shape[0]
    head_width = gain.shape[0]
    features = xs[0].shape[0]
    moved = len(weights) + len(xs) + len(kvs)
    q_shape = (heads, head_width, tile)
    return pl.pallas_call(
        first_kernel,
        out_shape=(
            jax.ShapeDtypeStruct((cores, tile // 2, heads * head_width), jnp.bfloat16),
            jax.ShapeDtypeStruct(q_shape, jnp.bfloat16),
        ),
        in_specs=[smem, smem, *[anywhere] * moved, vmem],
        out_specs=(vmem, vmem),
        scratch_shapes=[
            pltpu.VMEM(q_shape, jnp.bfloat16),
            pltpu.VMEM((features, heads * head_width), jnp.bfloat16),
            pltpu.VMEM((features, 2 * tile), jnp.bfloat16),
            pltpu.VMEM((len(kvs), *kvs[0].shape), jnp.bfloat16),
            pltpu.VMEM(q_shape, jnp.float32),
            pltpu.VMEM((heads, sublanes, tile), jnp.float32),
            pltpu.SemaphoreType.DMA((moved,)),
        ],
        cost_estimate=estimate(heads, head_width, features),
    )(place, offsets, *weights, *xs, *kvs, gain)


def attend_second(place, offsets, q_mine, kvs):
    heads, head_width = q_mine.shape[:2]
    return pl.pallas_call(
        second_kernel,
        out_shape=jax.ShapeDtypeStruct((cores, tile // 2, heads * head_width), jnp.bfloat16),
        in_specs=[smem, smem, vmem, *[anywhere] * len(kvs)],
        out_specs=vmem,
        scratch_shapes=[
            pltpu.VMEM((len(kvs), *kvs[0].shape), jnp.bfloat16),
            pltpu.VMEM(q_mine.shape, jnp.float32),
            pltpu.VMEM((heads, sublanes, tile), jnp.float32),
            pltpu.SemaphoreType.DMA((len(kvs),)),
        ],
        cost_estimate=estimate(heads, head_width, 0),
    )(place, offsets, q_mine, *kvs)


def sent_to_all(value, axes):
    count = lax.axis_size(axes)
    copies = jnp.broadcast_to(value, (count, *value.shape))
    return lax.all_to_all(copies, axes, split_axis=0, concat_axis=0, tiled=True)


def swapped(value, axis):
    return lax.ppermute(value, axis, [(0, 1), (1, 0)])


def turned(value, axis, shift):
    count = lax.axis_size(axis)
    return lax.ppermute(value, axis, [(i, (i + shift) % count) for i in range(count)])


def flipped(value, bits):
    return lax.ppermute(value, ("yl", "core"), [(i, i ^ bits) for i in range(group)])


def handed_on(value, shift):
    count = lax.axis_size("yh")
    return lax.ppermute(value, "yh", [(i, i + shift) for i in range(count - shift)])


def layer(stream, mix_gain, query_weight, query_gain, keys, key_gain, values, stick_offset):
    part, chip, core = lax.axis_index("yh"), lax.axis_index("yl"), lax.axis_index("core")
    member = chip * cores + core
    head_width = query_gain.shape[0]
    heads_all = stick_offset.shape[0]
    heads = heads_all // group
    rows_dev = query_weight.shape[0]
    padded = -(-rows_dev // 16) * 16
    span = heads * head_width
    tokens = stream.shape[1]

    columns = lax.dynamic_slice_in_dim(query_weight, member * span, span, 1)
    columns = jnp.pad(columns, ((0, padded - rows_dev), (0, 0)))
    along_z = sent_to_all(columns, "z").reshape(-1, span)

    kv_heads = keys.shape[2] // head_width

    def spread(rows):
        return rows.reshape(sublanes, tokens // sublanes, -1)[:, ::-1].swapaxes(0, 1)

    k = spread(keys[0]).reshape(tokens, kv_heads, head_width).astype(jnp.float32)
    k = k * lax.rsqrt(jnp.mean(k * k, axis=-1, keepdims=True) + norm_eps) * key_gain
    k = k.astype(jnp.bfloat16).transpose(1, 0, 2)
    v = spread(values[0]).reshape(tokens, kv_heads, head_width).transpose(1, 2, 0)
    kv = jnp.stack((k, v), axis=1)
    pieces = [lax.dynamic_index_in_dim(kv, member ^ bits, 0, keepdims=True) for bits in range(group)]
    pieces[1:] = [flipped(pieces[bits], bits) for bits in range(1, group)]
    kv_own = jnp.concatenate(pieces, axis=0)
    kvs = (kv_own, *[handed_on(kv_own, shift) for shift in range(1, lax.axis_size("yh"))])

    x_t = stream[0].T.astype(jnp.float32)
    scale = lax.rsqrt(jnp.mean(x_t * x_t, axis=0, keepdims=True) + norm_eps)
    normed = (x_t * scale * mix_gain[:, None]).astype(jnp.bfloat16)
    normed = normed.reshape(-1, low_x, rows_dev, tokens).transpose(1, 0, 2, 3)
    normed = jnp.pad(normed, ((0, 0), (0, 0), (0, padded - rows_dev), (0, 0)))
    normed = normed.reshape(-1, tokens)
    far = swapped(normed, "yl")
    near = swapped(normed, "core")
    both = swapped(far, "core")

    half = along_z.shape[0] // 2
    top, bottom = along_z[:half], along_z[half:]
    left_top = turned(top, "x", 1)
    right_bottom = turned(bottom, "x", -1)
    left_bottom = turned(bottom, "x", 1)
    right_top = turned(top, "x", -1)
    far_top = turned(left_top, "x", 1)
    far_bottom = turned(right_bottom, "x", -1)
    weights = (along_z, left_top, left_bottom, right_top, right_bottom, far_top, far_bottom)

    gain = query_gain * (head_width ** (-0.5) * log2_e)
    gain = jnp.broadcast_to(gain[:, None], (head_width, head_width))
    offsets = lax.dynamic_slice_in_dim(stick_offset * log2_e, member * heads, heads)
    place = jnp.stack((part, core, lax.axis_index("x"), member, chip)).astype(jnp.int32)
    xs = (far, both, normed, near)
    theirs, q_mine = attend_first(place, offsets, weights, xs, kvs, gain)
    arrived = swapped(theirs, "yl")
    ours = attend_second(place, offsets, q_mine, kvs)
    passed = swapped(jnp.stack((ours[1], arrived[1])), "core")
    pairs = (ours[0], passed[0]), (arrived[0], passed[1])
    (a, b), (c, d) = ((jnp.where(core == 0, p, q), jnp.where(core == 0, q, p)) for p, q in pairs)
    flip = chip == 0
    ordered = (jnp.where(flip, a, c), jnp.where(flip, b, d), jnp.where(flip, c, a), jnp.where(flip, d, b))
    return jnp.concatenate(ordered, axis=1)[None]


def solution(mesh):
    sp, dp = mesh.shape["sp"], mesh.shape["dp"]
    fine = Mesh(
        mesh.devices.reshape(sp // group, low_y, cores, dp // low_x, low_x),
        ("yh", "yl", "core", "z", "x"),
    )
    along, across = ("yh", "yl", "core"), ("z", "x")
    return jax.shard_map(
        layer,
        mesh=fine,
        in_specs=(
            P(across, along, None),
            P(),
            P(across, None),
            P(),
            P(across, along, None),
            P(),
            P(across, along, None),
            P(),
        ),
        out_specs=P(across, along, None),
        check_vma=False,
    )
```

```python
import jax
import jax.numpy as jnp
from jax import lax
from jax.experimental import pallas as pl
from jax.experimental.pallas import tpu as pltpu
from jax.sharding import Mesh, PartitionSpec as P


norm_eps = 1e-06
log2_e = 1.4426950408889634
tile = 256
sublanes = 8
low_y, cores, low_x = 2, 2, 4
group = low_y * cores


def sub_step(k, q, offset, carry, mask):
    scores = jnp.dot(k, q, preferred_element_type=jnp.float32)
    lanes = scores.shape[1]
    sub = lax.broadcasted_iota(jnp.int32, (sublanes, lanes), 0)
    kept, pieces = None, []
    for i in range(scores.shape[0] // sublanes):
        rows = slice(i * sublanes, (i + 1) * sublanes)
        odds = jnp.exp2(scores[rows] + offset)
        if mask is not None:
            odds = jnp.where(mask[rows], odds, 0.0)
        keep = 1.0 / (1.0 + odds)
        piece = odds * keep
        pieces.append(piece if kept is None else piece * kept)
        kept = keep if kept is None else kept * keep
    for j in (1, 2, 4):
        kept = kept * jnp.where(sub < sublanes - j, pltpu.roll(kept, sublanes - j, 0), 1.0)
    later = jnp.where(sub < sublanes - 1, pltpu.roll(kept, sublanes - 1, 0), 1.0) * carry
    carry = carry * jnp.broadcast_to(kept[0:1], kept.shape)
    weights = jnp.concatenate([piece * later for piece in pieces], axis=0)
    return weights.astype(jnp.bfloat16), carry


def block_step(k, v_t, q, offset, carry, mask):
    half = tile // 2
    upper, carry = sub_step(k[half:], q, offset, carry, None if mask is None else mask[half:])
    lower, carry = sub_step(k[:half], q, offset, carry, None if mask is None else mask[:half])
    part = jnp.dot(v_t[:, half:], upper, preferred_element_type=jnp.float32)
    part += jnp.dot(v_t[:, :half], lower, preferred_element_type=jnp.float32)
    return part, carry


def attend_kernel(
    place, offsets, w_own, w_left, w_left_end, w_right, w_right_end, w_far, w_far_end, x_own, x_core, x_far, x_both,
    kv_own, kv_one, kv_two, kv_three, gain, out_own, out_core, out_far, out_both, q_rows, total, carries,
):
    part, chip, core, column = place[0], place[1], place[2], place[3]
    member = chip * cores + core
    outs = (out_own, out_core, out_far, out_both)
    head_width = gain.shape[0]
    heads = offsets.shape[0]
    span = w_own.shape[0]
    half_span = w_far.shape[0]
    queries = None
    sources = (
        (w_own, 0, 0),
        (w_left, 3, 0),
        (w_left_end, 3, half_span),
        (w_right, 1, 0),
        (w_right_end, 1, half_span),
        (w_far, 2, 0),
        (w_far_end, 2, half_span),
    )
    for weight, shift, begin in sources:
        start = pl.multiple_of(lax.rem(column + shift, low_x) * span + begin, 16)
        rows = pl.ds(start, weight.shape[0])
        own, near, far, both = x_own[rows], x_core[rows], x_far[rows], x_both[rows]
        flip = core == 0
        wide = jnp.concatenate(
            [
                jnp.where(flip, own, near),
                jnp.where(flip, near, own),
                jnp.where(flip, far, both),
                jnp.where(flip, both, far),
            ],
            axis=1,
        )
        term = lax.dot_general(
            weight[...], wide, (((0,), (0,)), ((), ())), preferred_element_type=jnp.float32
        )
        queries = term if queries is None else queries + term
    for h in range(heads):
        for t in range(2):
            rows = queries[h * head_width : (h + 1) * head_width, t * tile : (t + 1) * tile]
            rows = rows.astype(jnp.bfloat16).astype(jnp.float32)
            mean = jnp.mean(rows * rows, axis=0, keepdims=True)
            scaled = rows * lax.rsqrt(mean + norm_eps) * gain[:, 0:1]
            q_rows[jnp.bitwise_xor(chip, t), h] = scaled.astype(jnp.bfloat16)
    row_id = lax.broadcasted_iota(jnp.int32, (tile, tile), 0)
    column_id = lax.broadcasted_iota(jnp.int32, (tile, tile), 1)
    half = tile // 2
    inner = row_id % half
    depth = half // sublanes
    key_id = row_id - inner + (inner % sublanes) * depth + (depth - 1 - inner // sublanes)
    mask = key_id < column_id

    def block_of(kv, index):
        left = kv[jnp.bitwise_xor(2 * index, member)]
        right = kv[jnp.bitwise_xor(2 * index + 1, member)]
        k = jnp.concatenate([left[0], right[0]], axis=0)
        return k, jnp.concatenate([left[1], right[1]], axis=1)

    one = jnp.ones((sublanes, tile), jnp.float32)
    first, last = block_of(kv_own, 0), block_of(kv_own, 1)
    for h in range(heads):
        offset = offsets[h]
        piece, carry = block_step(*last, q_rows[1, h], offset, one, mask)
        more, carry = block_step(*first, q_rows[1, h], offset, carry, None)
        total[h, 1] = piece + more
        carries[h, 1] = carry
        piece, carry = block_step(*first, q_rows[0, h], offset, one, mask)
        total[h, 0] = piece
        carries[h, 0] = carry

    for distance, kv in ((1, kv_one), (2, kv_two), (3, kv_three)):

        @pl.when(part >= distance)
        def _(kv=kv):
            blocks = (block_of(kv, 1), block_of(kv, 0))
            for h in range(heads):
                for t in range(2):
                    carry, summed = carries[h, t], total[h, t]
                    for k, v_t in blocks:
                        piece, carry = block_step(
                            k, v_t, q_rows[t, h], offsets[h], carry, None
                        )
                        summed = summed + piece
                    total[h, t] = summed
                    carries[h, t] = carry

    for h in range(heads):
        lanes = slice(h * head_width, (h + 1) * head_width)
        for t in range(2):
            rows = total[h, jnp.bitwise_xor(chip, t)].T.astype(jnp.bfloat16)
            low, high = rows[: tile // 2], rows[tile // 2 :]
            outs[2 * t][:, lanes] = jnp.where(core == 0, low, high)
            outs[2 * t + 1][:, lanes] = jnp.where(core == 0, high, low)


def attend(place, offsets, weights, xs, kvs, gain):
    heads = offsets.shape[0]
    head_width = gain.shape[0]
    vmem = pl.BlockSpec(memory_space=pltpu.VMEM)
    smem = pl.BlockSpec(memory_space=pltpu.SMEM)
    flops = 2 * xs[0].size * heads * head_width * group
    flops += heads * 8 * 2 * tile * tile * (2 * head_width + tile)
    return pl.pallas_call(
        attend_kernel,
        out_shape=[jax.ShapeDtypeStruct((tile // 2, heads * head_width), jnp.bfloat16)] * group,
        in_specs=[smem, smem, *[vmem] * 16],
        out_specs=[vmem] * group,
        scratch_shapes=[
            pltpu.VMEM((2, heads, head_width, tile), jnp.bfloat16),
            pltpu.VMEM((heads, 2, head_width, tile), jnp.float32),
            pltpu.VMEM((heads, 2, sublanes, tile), jnp.float32),
        ],
        cost_estimate=pl.CostEstimate(flops=flops, bytes_accessed=1 << 22, transcendentals=0),
    )(place, offsets, *weights, *xs, *kvs, gain)


def sent_to_all(value, axes):
    count = lax.axis_size(axes)
    copies = jnp.broadcast_to(value, (count, *value.shape))
    return lax.all_to_all(copies, axes, split_axis=0, concat_axis=0, tiled=True)


def swapped(value, axis):
    return lax.ppermute(value, axis, [(0, 1), (1, 0)])


def turned(value, axis, shift):
    count = lax.axis_size(axis)
    return lax.ppermute(value, axis, [(i, (i + shift) % count) for i in range(count)])


def flipped(value, bits):
    return lax.ppermute(value, ("yl", "core"), [(i, i ^ bits) for i in range(group)])


def handed_on(value, shift):
    count = lax.axis_size("yh")
    return lax.ppermute(value, "yh", [(i, i + shift) for i in range(count - shift)])


def layer(stream, mix_gain, query_weight, query_gain, keys, key_gain, values, stick_offset):
    part, chip, core = lax.axis_index("yh"), lax.axis_index("yl"), lax.axis_index("core")
    member = chip * cores + core
    head_width = query_gain.shape[0]
    heads_all = stick_offset.shape[0]
    heads = heads_all // group
    rows_dev = query_weight.shape[0]
    padded = -(-rows_dev // 16) * 16
    span = heads * head_width
    tokens = stream.shape[1]

    columns = lax.dynamic_slice_in_dim(query_weight, member * span, span, 1)
    columns = jnp.pad(columns, ((0, padded - rows_dev), (0, 0)))
    along_z = sent_to_all(columns, "z").reshape(-1, span)

    kv_heads = keys.shape[2] // head_width

    def spread(rows):
        return rows.reshape(sublanes, tokens // sublanes, -1)[:, ::-1].swapaxes(0, 1)

    k = spread(keys[0]).reshape(tokens, kv_heads, head_width).astype(jnp.float32)
    k = k * lax.rsqrt(jnp.mean(k * k, axis=-1, keepdims=True) + norm_eps) * key_gain
    k = k.astype(jnp.bfloat16).transpose(1, 0, 2)
    v = spread(values[0]).reshape(tokens, kv_heads, head_width).transpose(1, 2, 0)
    kv = jnp.stack((k, v), axis=1)
    pieces = [lax.dynamic_index_in_dim(kv, member ^ bits, 0, keepdims=True) for bits in range(group)]
    pieces[1:] = [flipped(pieces[bits], bits) for bits in range(1, group)]
    kv_own = jnp.concatenate(pieces, axis=0)
    kvs = (kv_own, *[handed_on(kv_own, shift) for shift in range(1, lax.axis_size("yh"))])

    x_t = stream[0].T.astype(jnp.float32)
    scale = lax.rsqrt(jnp.mean(x_t * x_t, axis=0, keepdims=True) + norm_eps)
    normed = (x_t * scale * mix_gain[:, None]).astype(jnp.bfloat16)
    normed = normed.reshape(-1, low_x, rows_dev, tokens).transpose(1, 0, 2, 3)
    normed = jnp.pad(normed, ((0, 0), (0, 0), (0, padded - rows_dev), (0, 0)))
    normed = normed.reshape(-1, tokens)
    far = swapped(normed, "yl")
    near = swapped(normed, "core")
    xs = (normed, near, far, swapped(far, "core"))

    half = along_z.shape[0] // 2
    top, bottom = along_z[:half], along_z[half:]
    left_top = turned(top, "x", 1)
    right_bottom = turned(bottom, "x", -1)
    left_bottom = turned(bottom, "x", 1)
    right_top = turned(top, "x", -1)
    far_top = turned(left_top, "x", 1)
    far_bottom = turned(right_bottom, "x", -1)
    weights = (along_z, left_top, left_bottom, right_top, right_bottom, far_top, far_bottom)

    gain = query_gain * (head_width ** (-0.5) * log2_e)
    gain = jnp.broadcast_to(gain[:, None], (head_width, head_width))
    place = jnp.stack((part, chip, core, lax.axis_index("x"))).astype(jnp.int32)
    offsets = lax.dynamic_slice_in_dim(stick_offset * log2_e, member * heads, heads)
    attended = attend(place, offsets, weights, xs, kvs, gain)
    third = flipped(attended[2], 2)
    fourth = flipped(attended[3], 3)
    second = flipped(attended[1], 1)
    pairs = (attended[0], second), (third, fourth)
    (a, b), (c, d) = ((jnp.where(core == 0, p, q), jnp.where(core == 0, q, p)) for p, q in pairs)
    flip = chip == 0
    ordered = (jnp.where(flip, a, c), jnp.where(flip, b, d), jnp.where(flip, c, a), jnp.where(flip, d, b))
    return jnp.concatenate(ordered, axis=1)[None]


def solution(mesh):
    sp, dp = mesh.shape["sp"], mesh.shape["dp"]
    fine = Mesh(
        mesh.devices.reshape(sp // group, low_y, cores, dp // low_x, low_x),
        ("yh", "yl", "core", "z", "x"),
    )
    along, across = ("yh", "yl", "core"), ("z", "x")
    return jax.shard_map(
        layer,
        mesh=fine,
        in_specs=(
            P(across, along, None),
            P(),
            P(across, None),
            P(),
            P(across, along, None),
            P(),
            P(across, along, None),
            P(),
        ),
        out_specs=P(across, along, None),
        check_vma=False,
    )
```
